32 devices in a mesh: sp: 8 (over z, x), tp: 4 (over y, core).
Axes of the slice: x: 2, y: 2, z: 4, core: 2. Of those that a mesh axis runs over, the one named last changes fastest.
Arguments:
- resid: bfloat16 [6144, 3072], P('sp', 'tp'), may hold values from -12 to 12
- query: bfloat16 [6144, 1536], P('sp', 'tp'), may hold values from -6 to 6
- keys: bfloat16 [6144, 1536], P('sp', 'tp'), may hold values from -6 to 6
- values: bfloat16 [6144, 1536], P('sp', 'tp'), may hold values from -6 to 6
- out_gate: bfloat16 [6144, 1536], P('sp', 'tp'), may hold values from -6 to 6
- in_gate: float32 [16, 6144], P('tp', 'sp'), may hold values from -6 to 110
- forget: float32 [16, 6144], P('tp', 'sp'), may hold values from -1 to 16
- doc_ids: int32 [6144], P('sp'), may hold values from 0 to 3, never falling along the last dimension, each value on 1 to 3072 neighbouring positions
- head_gain: float32 [1536], P('tp'), may hold values from 0.1 to 1.9
- w_out: bfloat16 [1536, 3072], P('tp'), may hold values from -0.15625 to 0.15625
- ffn_gain: float32 [3072], replicated, may hold values from 0.1 to 1.9
- w_gate: bfloat16 [3072, 8448], P('sp', 'tp'), may hold values from -0.109375 to 0.109375
- w_value: bfloat16 [3072, 8448], P('sp', 'tp'), may hold values from -0.109375 to 0.109375
- conv_taps: float32 [3, 8448], P(None, 'tp'), may hold values from -3.5 to 3.5
- w_down: bfloat16 [8448, 3072], P('tp', 'sp'), may hold values from -0.0625 to 0.0625
Outputs:
- layer_out: bfloat16 [6144, 3072], P('sp', 'tp')
The draws below stay inside these ranges and needn't reach their ends.
Inputs may be any that keep to these rules, and one draw needn't show every extreme that they name: `doc_ids`: document numbers never fall along the positions; each document is 1 to 3072 positions long.
All inputs are finite; a program needn't handle non-finite values.
Results may differ from the reference program's by a relative error of at most 0.02.
Values may be sent and summed in bfloat16 or wider, within the bound.
A program may use at most 128 MiB of HBM per device.

```python
import math
import jax
import jax.numpy as jnp
import numpy as np
from jax import lax

D = 3072
H = 16
DH = 96
FF = 8448
BLOCK = 64
TAPS = 3
TOK_DEV = 768
TOKENS = 6144
DOCS = 4
N_TP = 4


def draw_resid(key, part):
    base = jnp.clip(jax.random.normal(key, (TOKENS, D), jnp.float32), -6.0, 6.0)
    phase = jax.random.uniform(jax.random.fold_in(key, 1), (), jnp.float32, 0.0, 6.2832)
    columns = jnp.arange(D, dtype=jnp.float32)
    scale = 0.35 * jnp.exp(0.6 * jnp.sin(6.2832 * columns / D + phase))
    return (base * scale).astype(jnp.bfloat16)


def draw_in_gate(key, part):
    base = jnp.clip(jax.random.normal(key, (H, TOKENS), jnp.float32), -6.0, 6.0)
    return base


def draw_forget(key, part):
    limit = 4
    quick = jax.random.randint(jax.random.fold_in(key, 1), (H, 1), 0, 8) < limit
    rate = jnp.where(quick, 1.0 / 40.0, 1.0 / (4.0 * TOK_DEV))
    factor = jnp.exp(jax.random.uniform(jax.random.fold_in(key, 2), (H, TOKENS // 128), jnp.float32, -1.05, 1.05))
    factor = jnp.repeat(factor, 128, axis=1)
    noise = 0.5 * jnp.clip(jax.random.normal(jax.random.fold_in(key, 3), (H, TOKENS), jnp.float32), -6.0, 6.0)
    return -jnp.log(rate * factor) + noise


def steps_of(stream_key, extent, cuts, least, top_value):
    def one(position, blocks):
        draws = jax.random.uniform(jax.random.fold_in(jax.random.fold_in(stream_key, 6), position), (blocks,), jnp.float32, least / len(cuts), top_value / len(cuts))
        return jnp.repeat(jnp.exp(draws), extent[position] // blocks).reshape((-1,) + (1,) * (len(extent) - position - 1))

    gain = one(*cuts[0])
    for cut in cuts[1:]:
        gain = gain * one(*cut)
    return gain


def length_profile(count, total, most, skew):
    loads = [(1 << 20) // math.isqrt(rank ** skew) + 1 for rank in range(2, count + 1)]
    spare, counts = total - most - (count - 1), [1] * (count - 1)
    while spare > 0:
        free = [i for i in range(count - 1) if counts[i] < most]
        mass, remaining = sum([loads[i] for i in free]), spare
        for i in free:
            addition = min(most - counts[i], max(1, remaining * loads[i] // mass), spare)
            counts[i] = counts[i] + addition
            spare = spare - addition
    return np.array([most] + counts)


def uneven(stream_key, amount, total, reach, skew):
    if amount == 2:
        one = jax.random.randint(stream_key, (), max(1, total - reach), min(reach, total - 1) + 1)
        return jnp.stack([one, total - one])
    sizes = jnp.asarray(length_profile(amount, total, reach, skew), jnp.int32)
    pairs = (amount - 1) // 2
    giver, taker = sizes[1:1 + 2 * pairs:2], sizes[2:2 + 2 * pairs:2]
    margin = jnp.minimum(giver - 1, reach - taker)
    moved = jax.random.randint(jax.random.fold_in(stream_key, 1), (pairs,), 0, 1 << 20) % (margin + 1)
    sizes = sizes.at[1:1 + 2 * pairs:2].set(giver - moved).at[2:2 + 2 * pairs:2].set(taker + moved)
    return sizes[jax.random.permutation(jax.random.fold_in(stream_key, 2), amount)]


def centred(rng, dims, scale, most, shards=(), held_as=jnp.bfloat16):
    gain = steps_of(rng, dims, shards, -0.22, 0.18) if shards else 1.0
    entries = jax.random.normal(rng, dims, jnp.float32) * scale * gain
    return jnp.minimum(jnp.maximum(entries, -most), most).astype(held_as)


def setup_inputs(seed: int = 0) -> dict:
    splits = jax.random.split(jax.random.key(seed), 16)
    return {
        "resid": draw_resid(jax.random.fold_in(splits[15], 71), 0),
        "query": centred(splits[1], (TOKENS, H * DH), 1.0, 6.0, ((0, 8), (1, 4))),
        "keys": centred(splits[2], (TOKENS, H * DH), 1.0, 6.0, ((0, 8), (1, 4))),
        "values": centred(splits[3], (TOKENS, H * DH), 1.0, 6.0, ((0, 8), (1, 4))),
        "out_gate": centred(splits[4], (TOKENS, H * DH), 1.0, 6.0, ((0, 8), (1, 4))),
        "in_gate": draw_in_gate(jax.random.fold_in(splits[15], 71), 0),
        "forget": draw_forget(jax.random.fold_in(splits[15], 71), 0),
        "doc_ids": jnp.searchsorted(jnp.cumsum(uneven(splits[7], DOCS, TOKENS, 4 * TOK_DEV, 0)), jnp.arange(TOKENS), side="right").astype(jnp.int32),
        "head_gain": jnp.clip(1.0 + 0.18 * jax.random.normal(splits[8], (H * DH,), jnp.float32), 0.1, 1.9),
        "w_out": centred(splits[9], (H * DH, D), (H * DH) ** -0.5, 0.15625, ((0, 4),)),
        "ffn_gain": jnp.clip(1.0 + 0.18 * jax.random.normal(splits[10], (D,), jnp.float32), 0.1, 1.9),
        "w_gate": centred(splits[11], (D, FF), D ** -0.5, 0.109375, ((0, 8), (1, 4))),
        "w_value": centred(splits[12], (D, FF), D ** -0.5, 0.109375, ((0, 8), (1, 4))),
        "conv_taps": centred(splits[13], (TAPS, FF), TAPS ** -0.5, 3.5, ((1, 4),), jnp.float32),
        "w_down": centred(splits[14], (FF, D), FF ** -0.5, 0.0625, ((0, 4), (1, 8))),
    }


ABSENT = -1e+30
epsilon = 1e-06
head_floor = 1.0
HIGHEST = lax.Precision.HIGHEST

def combine(early, late):
    state_early, peak_early, decay_early, first_early, last_early, second_early = early
    state_late, peak_late, decay_late, first_late, last_late, second_late = late
    early_empty = last_early < 0.0
    late_empty = first_late < 0.0
    cut = (first_late != last_early) & jnp.logical_not(early_empty) & jnp.logical_not(late_empty)
    passed = jnp.where(cut, ABSENT, decay_late)
    peak = jnp.maximum(passed + peak_early, peak_late)
    keep = jnp.exp(passed + peak_early - peak)
    fresh = jnp.exp(peak_late - peak)
    state = keep[..., None, None] * state_early + fresh[..., None, None] * state_late
    return (state, peak, decay_early + passed, jnp.where(early_empty, first_late, first_early), jnp.where(late_empty, last_early, last_late), jnp.where(late_empty, second_early, second_late))

def empty_state(heads, width):
    return (jnp.zeros((heads, width, width), jnp.float32), jnp.full((heads,), ABSENT, jnp.float32), jnp.zeros((heads,), jnp.float32), jnp.full((1,), -1.0, jnp.float32), jnp.full((1,), -1.0, jnp.float32), jnp.full((1,), -1.0, jnp.float32))

def advance(carry, item):
    return (combine(carry, item), carry)

def block_parts(query, keys, values, in_gate, forget, seg):
    length, heads, width = query.shape
    count = length // BLOCK
    query_blocks = query.reshape(count, BLOCK, heads, width)
    key_blocks = (keys * width ** (-0.5)).reshape(count, BLOCK, heads, width)
    value_blocks = values.reshape(count, BLOCK, heads, width)
    gate_in = in_gate.T.reshape(count, BLOCK, heads)
    cumul = jnp.cumsum(jax.nn.log_sigmoid(forget.T).reshape(count, BLOCK, heads), axis=1)
    seg_blocks = seg.reshape(count, BLOCK)
    total = cumul[:, -1]
    in_last = (seg_blocks == seg_blocks[:, -1:])[:, :, None]
    weight_log = jnp.where(in_last, total[:, None] - cumul + gate_in, ABSENT)
    local_peak = lax.optimization_barrier(jnp.max(weight_log, axis=1))
    weights = jnp.exp(weight_log - local_peak[:, None])
    update = jnp.einsum('nchk,nchv->nhkv', weights[..., None] * key_blocks, value_blocks, precision=HIGHEST)
    whole = jnp.all(seg_blocks == seg_blocks[:, :1], axis=1)[:, None]
    decay = jnp.where(whole, total, ABSENT)
    elements = (update, local_peak, decay, seg_blocks[:, :1], seg_blocks[:, -1:], seg_blocks[:, -2:-1])
    return (elements, (query_blocks, key_blocks, value_blocks, gate_in, cumul, seg_blocks))

def block_outputs(before, parts):
    state, peak_prev, _, _, last_prev, _ = before
    query_blocks, key_blocks, value_blocks, gate_in, cumul, seg_blocks = parts
    count, span, heads, width = query_blocks.shape
    carried = (seg_blocks == last_prev)[:, :, None]
    inter = jnp.where(carried, cumul + peak_prev[:, None], ABSENT)
    places = jnp.arange(span)
    causal = (places[:, None] >= places[None, :])[None, :, :, None]
    same = (seg_blocks[:, :, None] == seg_blocks[:, None, :])[..., None]
    diff_log = jnp.where(causal & same, cumul[:, :, None] - cumul[:, None] + gate_in[:, None], ABSENT)
    top = jnp.maximum(inter, lax.optimization_barrier(jnp.max(diff_log, axis=2)))
    scores = jnp.einsum('nthd,nshd->ntsh', query_blocks, key_blocks, precision=HIGHEST) * jnp.exp(diff_log - top[:, :, None])
    result = jnp.einsum('ntsh,nshd->nthd', scores, value_blocks, precision=HIGHEST)
    result = result + jnp.exp(inter - top)[..., None] * jnp.einsum('nthk,nhkv->nthv', query_blocks, state, precision=HIGHEST)
    return result.reshape(count * span, heads, width)

def reference(resid, query, keys, values, out_gate, in_gate, forget, doc_ids, head_gain, w_out, ffn_gain, w_gate, w_value, conv_taps, w_down):
    length = query.shape[0]
    seg = doc_ids.astype(jnp.float32)
    query_f = query.astype(jnp.float32).reshape(length, H, DH)
    keys_f = keys.astype(jnp.float32).reshape(length, H, DH)
    values_f = values.astype(jnp.float32).reshape(length, H, DH)
    elements, parts = block_parts(query_f, keys_f, values_f, in_gate, forget, seg)
    _, before = lax.scan(advance, empty_state(H, DH), elements)
    memory_out = block_outputs(before, parts)
    normed = memory_out * lax.rsqrt(lax.optimization_barrier(jnp.mean(memory_out * memory_out, axis=-1, keepdims=True)) + head_floor)
    normed = normed.reshape(length, H * DH) * head_gain * jax.nn.sigmoid(out_gate.astype(jnp.float32))
    mix = normed.astype(jnp.bfloat16)
    width_group = H // N_TP * DH
    attended = jnp.zeros((length, D), jnp.float32)
    for index in range(N_TP):
        share = jnp.dot(mix[:, index * width_group:(index + 1) * width_group], w_out[index * width_group:(index + 1) * width_group], preferred_element_type=jnp.float32).astype(jnp.bfloat16)
        attended = attended + lax.optimization_barrier(share).astype(jnp.float32)
    residual_one = resid.astype(jnp.float32) + attended
    scale = lax.rsqrt(lax.optimization_barrier(jnp.mean(residual_one * residual_one, axis=1, keepdims=True)) + epsilon)
    normed_rows = (residual_one * scale * ffn_gain).astype(jnp.bfloat16)
    gate = jnp.dot(normed_rows, w_gate, preferred_element_type=jnp.float32).astype(jnp.bfloat16)
    value = jnp.dot(normed_rows, w_value, preferred_element_type=jnp.float32).astype(jnp.bfloat16)
    extended = jnp.concatenate([jnp.zeros((2, FF), jnp.bfloat16), gate], axis=0).astype(jnp.float32)
    ids = jnp.concatenate([jnp.full((2,), -1.0, jnp.float32), seg])
    near = (ids[1:-1] == seg)[:, None]
    far = (ids[:-2] == seg)[:, None]
    conv = conv_taps[2] * extended[2:] + conv_taps[1] * jnp.where(near, extended[1:-1], 0.0) + conv_taps[0] * jnp.where(far, extended[:-2], 0.0)
    hidden = (jax.nn.silu(conv) * value.astype(jnp.float32)).astype(jnp.bfloat16)
    group = FF // N_TP
    down = jnp.zeros((length, D), jnp.float32)
    for index in range(N_TP):
        partial_rows = jnp.dot(hidden[:, index * group:(index + 1) * group], w_down[index * group:(index + 1) * group], preferred_element_type=jnp.float32).astype(jnp.bfloat16)
        down = down + lax.optimization_barrier(partial_rows).astype(jnp.float32)
    return (residual_one + down).astype(jnp.bfloat16)
```

```python
import jax
import jax.numpy as jnp
from jax import lax
from jax.experimental import pallas as pl
from jax.experimental.pallas import tpu as pltpu
from jax.sharding import PartitionSpec as P

MESH = pl.DeviceIdType.MESH
DH = 96
ZS = 4
ABSENT = -1e30
epsilon = 1e-06
head_floor = 1.0


def front(query, keys, values, out_gate, in_gate, forget, doc_ids, head_gain, w_out, resid, ffn_gain, wg, wv):
    tokens, width = query.shape
    heads = in_gate.shape[0]
    own_cols = resid.shape[1]
    n_sp, n_tp = lax.axis_size("sp"), lax.axis_size("tp")
    X, Y = n_sp // ZS, n_tp // 2
    units, depth = wg.shape
    half = units // 2
    merged = depth % 128 == 0 and X * depth == own_cols
    per = n_sp // n_tp
    full = own_cols * n_tp
    tile = 256 if tokens % 256 == 0 else tokens
    tiles = tokens // tile
    srows = heads * DH + 24
    steps = []
    d = 1
    while d < tokens:
        steps.append(d)
        d *= 2
    w_shape = (ZS, 2, half, X * depth) if merged else (ZS, 2, X, half, depth)

    def kernel(
        q_ref, k_ref, v_ref, og_ref, ig_ref, fg_ref, doc_ref, hg_ref, wo_hbm, res_ref, gain_ref, wg_hbm, wv_hbm,
        gate_ref, value_ref, resid_ref, mask_ref,
        w, rows, acc, wo, mixes, local, states, small, cols, cols2, pad, carry, sin, sq, sqb,
        z_send, z_recv, x_send, x_recv, own_sem, wo_send, wo_recv, wo_own,
        st_send, st_recv, mix_send, mix_recv, sq_send, sq_recv, ra_send, ra_recv, rb_send, rb_recv, rz_send, rz_recv, mk_send, mk_recv,
    ):
        me, t = lax.axis_index("sp"), lax.axis_index("tp")
        z, col = me // X, me % X
        side = z % 2
        y, core = t // 2, t % 2
        sib = t + 1 - 2 * core
        zs = [z, z + 1 - 2 * side, (z + 2) % 4, 3 - z]
        halves = [side, 1 - side, side, 1 - side]

        def sp_dev(i):
            return {"sp": i, "tp": t}

        def tp_dev(i):
            return {"sp": me, "tp": i}

        barrier = pltpu.get_barrier_semaphore()
        for i in range(1, n_sp):
            pl.semaphore_signal(barrier, inc=1, device_id=sp_dev((me + i) % n_sp), device_id_type=MESH)
        for i in range(1, n_tp):
            pl.semaphore_signal(barrier, inc=1, device_id=tp_dev((t + i) % n_tp), device_id_type=MESH)
        pl.semaphore_wait(barrier, n_sp + n_tp - 2)

        hbm = (wg_hbm, wv_hbm)

        def lanes(c):
            return pl.ds(pl.multiple_of(c * depth, depth), depth)

        def slot(zi, part, c):
            if merged:
                return w.at[zi, part, :, lanes(c)]
            return w.at[zi, part, c]

        def half_of(part, s):
            return hbm[part].at[pl.ds(pl.multiple_of(s * half, 16), half), :]

        def z_copy(j, part):
            return pltpu.make_async_remote_copy(
                src_ref=half_of(part, halves[j]), dst_ref=slot(z, part, col),
                send_sem=z_send.at[j - 1, part], recv_sem=z_recv.at[j - 1, part],
                device_id=sp_dev(zs[j] * X + col), device_id_type=MESH)

        def z_wait(j, part):
            pltpu.make_async_remote_copy(
                src_ref=half_of(part, halves[j]), dst_ref=slot(zs[j], part, col),
                send_sem=z_send.at[j - 1, part], recv_sem=z_recv.at[j - 1, part],
                device_id=sp_dev(zs[j] * X + col), device_id_type=MESH).wait_recv()

        def x_copy(j, part, by):
            src = half_of(part, side) if j == 0 else slot(zs[j], part, col)
            return pltpu.make_async_remote_copy(
                src_ref=src, dst_ref=slot(zs[j], part, col),
                send_sem=x_send.at[j, part, by - 1], recv_sem=x_recv.at[j, part, by - 1],
                device_id=sp_dev(z * X + (col + by) % X), device_id_type=MESH)

        def x_start(j, part):
            for by in range(1, X):
                x_copy(j, part, by).start()

        def relay(j, part):
            z_wait(j, part)
            x_start(j, part)

        def x_wait(j, part):
            for by in range(1, X):
                there = slot(zs[j], part, (col + X - by) % X)
                pltpu.make_async_remote_copy(
                    src_ref=there, dst_ref=there,
                    send_sem=x_send.at[j, part, by - 1], recv_sem=x_recv.at[j, part, by - 1],
                    device_id=sp_dev(z * X + (col + by) % X), device_id_type=MESH).wait_recv()

        z_copy(1, 0).start()
        x_start(0, 0)
        for part in range(2):
            pltpu.make_async_copy(half_of(part, side), slot(z, part, col), own_sem.at[part]).start()

        def wo_cols(i):
            return wo_hbm.at[:, pl.ds(pl.multiple_of(i * own_cols, own_cols), own_cols)]

        def wo_rows(i):
            return wo.at[pl.ds(pl.multiple_of(i * width, 16), width), :]

        def wo_copy(i):
            peer = (t + i) % n_tp
            return pltpu.make_async_remote_copy(
                src_ref=wo_cols(peer), dst_ref=wo_rows(t),
                send_sem=wo_send.at[i - 1], recv_sem=wo_recv.at[i - 1],
                device_id=tp_dev(peer), device_id_type=MESH)

        def wo_wait(i):
            there = wo_rows((t + n_tp - i) % n_tp)
            pltpu.make_async_remote_copy(
                src_ref=there, dst_ref=there, send_sem=wo_send.at[i - 1], recv_sem=wo_recv.at[i - 1],
                device_id=tp_dev((t + i) % n_tp), device_id_type=MESH).wait_recv()

        for i in range(1, n_tp):
            wo_copy(i).start()
        pltpu.make_async_copy(wo_cols(t), wo_rows(t), wo_own).start()

        lane = lax.broadcasted_iota(jnp.int32, (8, tokens), 1)
        pad[...] = jnp.zeros_like(pad)
        small[...] = jnp.zeros_like(small)
        pad[0, 0:heads, :] = ig_ref[...]
        pad[1, 0:heads, :] = fg_ref[...]
        gin, f = pad[0], pad[1]
        c = jnp.minimum(f, 0.0) - jnp.log1p(jnp.exp(-jnp.abs(f)))
        seg = jnp.broadcast_to(doc_ref[...].astype(jnp.float32), (8, tokens))
        for d in steps:
            c = c + jnp.where(lane >= d, pltpu.roll(c, d, 1), 0.0)
        b = gin - c
        m = b
        for d in steps:
            ok = (lane >= d) & (pltpu.roll(seg, d, 1) == seg)
            m = jnp.where(ok, jnp.maximum(m, pltpu.roll(m, d, 1)), m)
        c_last, m_last, s_last = c[:, tokens - 1 :], m[:, tokens - 1 :], seg[:, tokens - 1 :]
        s_second = seg[:, tokens - 2 : tokens - 1]
        weight = jnp.where(seg == s_last, jnp.exp(jnp.minimum(b - m_last, 0.0)), 0.0)
        small[0:8] = m
        small[8:16] = weight
        small[16:24] = seg
        small[24:32] = b
        small[32:40] = c
        cols[...] = small[...].T

        for h in range(heads):
            part = slice(h * DH, (h + 1) * DH)
            weighted = (k_ref[:, part].astype(jnp.float32) * cols[:, 8 + h : 9 + h]).astype(jnp.bfloat16)
            states[me, h * DH : (h + 1) * DH, :] = lax.dot_general(
                weighted, v_ref[:, part], (((0,), (0,)), ((), ())), preferred_element_type=jnp.float32
            ) * (DH ** -0.5)
        base = heads * DH
        states[me, base : base + 8, :] = jnp.broadcast_to(c_last + m_last, (8, DH))
        states[me, base + 8 : base + 16, :] = jnp.broadcast_to(c_last, (8, DH))
        first_lane = lax.broadcasted_iota(jnp.int32, (8, DH), 1) == 0
        states[me, base + 16 : base + 24, :] = jnp.where(
            first_lane, jnp.broadcast_to(s_last, (8, DH)), jnp.broadcast_to(s_second, (8, DH)))

        def st_copy(d):
            return pltpu.make_async_remote_copy(
                src_ref=states.at[me], dst_ref=states.at[me],
                send_sem=st_send.at[d - 1], recv_sem=st_recv.at[d - 1],
                device_id=sp_dev((me + d) % n_sp), device_id_type=MESH)

        for d in range(1, n_sp):
            pl.when(me + d < n_sp)(lambda d=d: st_copy(d).start())
        z_copy(1, 1).start()
        x_start(0, 1)
        z_copy(2, 0).start()

        for i in range(tiles):
            span = (i + 1) * tile
            at = slice(i * tile, span)
            tpos = lax.broadcasted_iota(jnp.int32, (tile, span), 0) + i * tile
            spos = lax.broadcasted_iota(jnp.int32, (tile, span), 1)
            allowed = (tpos >= spos) & (cols[at, 16:17] == small[16:17, 0:span])
            for h in range(heads):
                part = slice(h * DH, (h + 1) * DH)
                log = jnp.where(allowed, small[24 + h : 25 + h, 0:span] - cols[at, h : h + 1], ABSENT)
                scores = lax.dot_general(
                    q_ref[at, part], k_ref[0:span, part], (((1,), (1,)), ((), ())), preferred_element_type=jnp.float32)
                scores = (scores * jnp.exp(log)).astype(jnp.bfloat16)
                local[at, part] = jnp.dot(scores, v_ref[0:span, part], preferred_element_type=jnp.float32) * (DH ** -0.5)

        relay(1, 0)

        carry[0] = jnp.zeros((8, DH), jnp.float32)
        carry[1] = jnp.full((8, DH), ABSENT, jnp.float32)
        carry[2] = jnp.full((8, DH), -1.0, jnp.float32)
        sin[...] = jnp.zeros_like(sin)

        def earlier(d):
            there = states.at[(me + n_sp - d) % n_sp]
            pltpu.make_async_remote_copy(
                src_ref=there, dst_ref=there, send_sem=st_send.at[d - 1], recv_sem=st_recv.at[d - 1],
                device_id=sp_dev((me + d) % n_sp), device_id_type=MESH).wait_recv()
            block = states[(me + n_sp - d) % n_sp, base : base + 24, :]
            peak, total, ends = block[0:8], block[8:16], block[16:24]
            if d == 1:
                carry[2] = ends
            use = ends[:, 0:1] == carry[2][:, 0:1]
            logs = jnp.where(use, peak + carry[0], ABSENT)
            carry[2 + d] = logs
            carry[1] = jnp.maximum(carry[1], logs)
            carry[0] = carry[0] + total

        for d in range(1, n_sp):
            pl.when(me >= d)(lambda d=d: earlier(d))

        def add_state(d):
            coef = jnp.exp(carry[2 + d] - carry[1])
            for h in range(heads):
                at = slice(h * DH, (h + 1) * DH)
                sin[at, :] = sin[at, :] + coef[h : h + 1, :] * states[(me + n_sp - d) % n_sp, at, :]

        for d in range(1, n_sp):
            pl.when(me >= d)(lambda d=d: add_state(d))

        peak_in = carry[1][:, 0:1]
        last_prev = carry[2][:, 0:1]
        second_prev = carry[2][:, 1:2]
        c, m, seg = small[32:40], small[0:8], small[16:24]
        inter = jnp.where(seg == last_prev, c + peak_in, ABSENT)
        top = c + m
        peak_all = jnp.maximum(inter, top)
        before = jnp.where(lane == 0, last_prev, pltpu.roll(seg, 1, 1))
        before2 = jnp.where(lane == 0, second_prev, jnp.where(lane == 1, last_prev, pltpu.roll(seg, 2, 1)))
        row = lax.broadcasted_iota(jnp.int32, (8, tokens), 0)
        mask_ref[0] = jnp.where(jnp.where(row == 0, before, before2) == seg, 1.0, 0.0)
        small[40:48] = jnp.exp(top - peak_all)
        small[48:56] = jnp.exp(inter - peak_all)
        cols2[...] = small[...].T

        for i in range(tiles):
            at = slice(i * tile, (i + 1) * tile)
            for h in range(heads):
                part = slice(h * DH, (h + 1) * DH)
                out = cols2[at, 40 + h : 41 + h] * local[at, part] + cols2[at, 48 + h : 49 + h] * jnp.dot(
                    q_ref[at, part], sin[part, :].astype(jnp.bfloat16), preferred_element_type=jnp.float32)
                local[at, part] = out * lax.rsqrt(jnp.mean(out * out, axis=-1, keepdims=True) + head_floor)
            mixes[t, at, :] = (
                local[at, :] * hg_ref[...] * jax.nn.sigmoid(og_ref[at, :].astype(jnp.float32))
            ).astype(jnp.bfloat16)

        def gather(at, send, recv):
            def copy(index, source, dest):
                return pltpu.make_async_remote_copy(
                    src_ref=at(source), dst_ref=at(source), send_sem=send.at[index], recv_sem=recv.at[index],
                    device_id=tp_dev(dest), device_id_type=MESH)

            def start():
                copy(0, t, sib).start()
                for j in range(1, Y):
                    copy(j, t, ((y + j) % Y) * 2 + core).start()

            def forward():
                for j in range(1, Y):
                    source = ((y + Y - j) % Y) * 2 + core
                    copy(j, source, sib).wait_recv()
                    copy(Y - 1 + j, source, sib).start()

            def finish():
                copy(0, sib, sib).wait_recv()
                for j in range(1, Y):
                    copy(Y - 1 + j, ((y + Y - j) % Y) * 2 + 1 - core, sib).wait_recv()

            def sent():
                copy(0, t, sib).wait_send()
                for j in range(1, Y):
                    copy(j, t, sib).wait_send()
                    copy(Y - 1 + j, t, sib).wait_send()

            return start, forward, finish, sent

        mix_g = gather(lambda i: mixes.at[i], mix_send, mix_recv)
        mix_g[0]()
        relay(1, 1)
        mix_g[1]()
        for i in range(1, n_tp):
            wo_wait(i)
        pltpu.make_async_copy(wo_cols(t), wo_rows(t), wo_own).wait()
        mix_g[2]()

        def project(i, _):
            at = pl.ds(pl.multiple_of(i * tile, tile), tile)
            total = res_ref[at, :].astype(jnp.float32)
            for s in range(n_tp):
                total = total + jnp.dot(
                    mixes[s, at, :], wo[s * width : (s + 1) * width, :], preferred_element_type=jnp.float32)
            resid_ref[at, :] = total
            cols2[at, :] = jnp.broadcast_to(jnp.sum(total * total, axis=1, keepdims=True), (tile, 128))
            return 0

        lax.fori_loop(0, tiles, project, 0)
        sq[t] = cols2[...].T[0:8]

        def sq_copy(i):
            return pltpu.make_async_remote_copy(
                src_ref=sq.at[t], dst_ref=sq.at[t], send_sem=sq_send.at[i - 1], recv_sem=sq_recv.at[i - 1],
                device_id=tp_dev((t + i) % n_tp), device_id_type=MESH)

        for i in range(1, n_tp):
            sq_copy(i).start()
        for i in range(1, n_tp):
            there = sq.at[(t + n_tp - i) % n_tp]
            pltpu.make_async_remote_copy(
                src_ref=there, dst_ref=there, send_sem=sq_send.at[i - 1], recv_sem=sq_recv.at[i - 1],
                device_id=tp_dev((t + i) % n_tp), device_id_type=MESH).wait_recv()
        squares = sq[0]
        for s in range(1, n_tp):
            squares = squares + sq[s]
        small[0:8] = lax.rsqrt(squares / full + epsilon)
        cols2[...] = small[...].T

        def normalize(i, _):
            at = pl.ds(pl.multiple_of(i * tile, tile), tile)
            rows[t, at, :] = (resid_ref[at, :] * cols2[at, 0:1] * gain_ref[t]).astype(jnp.bfloat16)
            return 0

        lax.fori_loop(0, tiles, normalize, 0)

        mine, theirs = pl.ds(0, tokens), pl.ds(tokens, tokens)
        ra = gather(lambda i: rows.at[i, mine], ra_send, ra_recv)
        rb = gather(lambda i: rows.at[i, theirs], rb_send, rb_recv)
        partner = sp_dev(zs[1] * X + col)
        rz = pltpu.make_async_remote_copy(
            src_ref=rows.at[t, mine], dst_ref=rows.at[t, theirs], send_sem=rz_send, recv_sem=rz_recv,
            device_id=partner, device_id_type=MESH)
        mk = pltpu.make_async_remote_copy(
            src_ref=mask_ref.at[0], dst_ref=mask_ref.at[1], send_sem=mk_send, recv_sem=mk_recv,
            device_id=partner, device_id_type=MESH)
        ra[0]()
        rz.start()
        mk.start()
        z_copy(2, 1).start()
        z_copy(3, 0).start()
        z_copy(3, 1).start()
        relay(2, 0)
        ra[1]()
        rz.wait_recv()
        rb[0]()
        ra[2]()

        def ready(j):
            for part in range(2):
                if j == 0:
                    pltpu.make_async_copy(half_of(part, side), slot(z, part, col), own_sem.at[part]).wait()
                x_wait(j, part)

        def multiply(j, blocks, begin, end):
            def body(i, _):
                at = pl.ds(pl.multiple_of(i * tile, tile), tile)
                for part, out in enumerate((gate_ref, value_ref)):
                    total = None if begin else acc[part, at, :]
                    for zi in [zs[k] for k in j]:
                        if merged:
                            terms = [(rows[zi, at, :], w[zi, part])]
                        else:
                            terms = [
                                (rows[zi * (X // per) + x // per, at, (x % per) * depth : (x % per + 1) * depth],
                                 w[zi, part, x])
                                for x in range(X)
                            ]
                        for left, right in terms:
                            term = lax.dot_general(
                                left, right, (((1,), (1,)), ((), ())), preferred_element_type=jnp.float32)
                            total = term if total is None else total + term
                    if end:
                        out[at, :] = total.astype(jnp.bfloat16)
                    else:
                        acc[part, at, :] = total
                return 0

            lax.fori_loop(blocks[0] * tiles, blocks[1] * tiles, body, 0)

        ready(0)
        ready(1)
        multiply((0, 1), (0, 1), True, False)
        relay(2, 1)
        rb[1]()
        rb[2]()
        multiply((0, 1), (1, 2), True, False)
        relay(3, 0)
        ready(2)
        multiply((2,), (0, 2), False, False)
        relay(3, 1)
        ready(3)
        multiply((3,), (0, 2), False, True)

        for part in range(2):
            for j in range(1, 4):
                z_copy(j, part).wait_send()
            for j in range(4):
                for by in range(1, X):
                    x_copy(j, part, by).wait_send()
        for i in range(1, n_tp):
            wo_copy(i).wait_send()
            sq_copy(i).wait_send()
        for d in range(1, n_sp):
            pl.when(me + d < n_sp)(lambda d=d: st_copy(d).wait_send())
        mix_g[3]()
        ra[3]()
        rb[3]()
        rz.wait_send()
        mk.wait()

    vmem = pl.BlockSpec(memory_space=pltpu.VMEM)
    hbm_spec = pl.BlockSpec(memory_space=pl.ANY)
    dma = pltpu.SemaphoreType.DMA
    bf16, f32 = jnp.bfloat16, jnp.float32
    return pl.pallas_call(
        kernel,
        in_specs=[vmem] * 8 + [hbm_spec] + [vmem] * 2 + [hbm_spec] * 2,
        out_specs=[vmem] * 4,
        out_shape=[
            jax.ShapeDtypeStruct((2 * tokens, half), bf16),
            jax.ShapeDtypeStruct((2 * tokens, half), bf16),
            jax.ShapeDtypeStruct((tokens, own_cols), f32),
            jax.ShapeDtypeStruct((2, 8, tokens), f32),
        ],
        scratch_shapes=[
            pltpu.VMEM(w_shape, bf16),
            pltpu.VMEM((n_tp, 2 * tokens, own_cols), bf16),
            pltpu.VMEM((2, 2 * tokens, half), f32),
            pltpu.VMEM((n_tp * width, own_cols), bf16),
            pltpu.VMEM((n_tp, tokens, width), bf16),
            pltpu.VMEM((tokens, width), f32),
            pltpu.VMEM((n_sp, srows, DH), f32),
            pltpu.VMEM((128, tokens), f32),
            pltpu.VMEM((tokens, 128), f32),
            pltpu.VMEM((tokens, 128), f32),
            pltpu.VMEM((2, 8, tokens), f32),
            pltpu.VMEM((2 + n_sp, 8, DH), f32),
            pltpu.VMEM((heads * DH, DH), f32),
            pltpu.VMEM((n_tp, 8, tokens), f32),
            pltpu.VMEM((8, 128), f32),
            dma((3, 2)), dma((3, 2)),
            dma((4, 2, X - 1)), dma((4, 2, X - 1)),
            dma((2,)),
            dma((n_tp - 1,)), dma((n_tp - 1,)), dma,
            dma((n_sp - 1,)), dma((n_sp - 1,)),
            dma((n_tp - 1,)), dma((n_tp - 1,)),
            dma((n_tp - 1,)), dma((n_tp - 1,)),
            dma((n_tp - 1,)), dma((n_tp - 1,)),
            dma((n_tp - 1,)), dma((n_tp - 1,)),
            dma, dma, dma, dma,
        ],
        compiler_params=pltpu.CompilerParams(
            vmem_limit_bytes=67043328, collective_id=0, has_side_effects=True),
        name="front",
    )(
        query, keys, values, out_gate, in_gate, forget, doc_ids[None], head_gain[None], w_out, resid,
        ffn_gain.reshape(n_tp, 1, own_cols), wg, wv,
    )


def down_product(hidden, blocks):
    tokens, depth = hidden.shape
    columns = blocks[0][0].shape[1]
    count = len(blocks)
    tile = tokens // 3
    index = jnp.stack([place for _, place in blocks]).astype(jnp.int32)

    def kernel(index_ref, rows, *rest):
        sources, out, weights, sems = rest[:count], rest[count], rest[count + 1], rest[count + 2]

        @pl.when(pl.program_id(0) == 0)
        def _():
            copies = [
                pltpu.make_async_copy(sources[k], weights.at[index_ref[k]], sems.at[k])
                for k in range(count)
            ]
            for copy in copies:
                copy.start()
            for copy in copies:
                copy.wait()

        for k in range(count):
            out[k] = jnp.dot(
                rows[...], weights[k], preferred_element_type=jnp.float32
            ).astype(jnp.bfloat16)

    return pl.pallas_call(
        kernel,
        grid_spec=pltpu.PrefetchScalarGridSpec(
            num_scalar_prefetch=1,
            grid=(tokens // tile,),
            in_specs=[pl.BlockSpec((tile, depth), lambda i, index: (i, 0))]
            + [pl.BlockSpec(memory_space=pl.ANY)] * count,
            out_specs=pl.BlockSpec((count, tile, columns), lambda i, index: (0, i, 0)),
            scratch_shapes=[
                pltpu.VMEM((count, depth, columns), jnp.bfloat16),
                pltpu.SemaphoreType.DMA((count,)),
            ],
        ),
        out_shape=jax.ShapeDtypeStruct((count, tokens, columns), jnp.bfloat16),
        compiler_params=pltpu.CompilerParams(vmem_limit_bytes=40 << 20),
        cost_estimate=pl.CostEstimate(
            flops=2 * tokens * depth * count * columns,
            bytes_accessed=2 * count * columns * (tokens + depth),
            transcendentals=0,
        ),
        name="lowered",
    )(index, hidden, *[block for block, _ in blocks])


def layer(
    resid,
    query,
    keys,
    values,
    out_gate,
    in_gate,
    forget,
    doc_ids,
    head_gain,
    w_out,
    ffn_gain,
    w_gate,
    w_value,
    conv_taps,
    w_down,
):
    tokens = query.shape[0]
    count = lax.axis_size("sp")
    me = lax.axis_index("sp")
    across = count // 4
    side = (me // across) % 2
    first = side == 0
    column = me % across
    hidden_units = w_gate.shape[1]
    half = hidden_units // 2

    def flip(value, bit):
        return lax.ppermute(value, "sp", [(s, s ^ bit) for s in range(count)])

    def shift(value, by):
        return lax.ppermute(
            value,
            "sp",
            [(s, s - s % across + (s % across + by) % across) for s in range(count)],
        )

    gate_both, value_both, residual_own, masks_both = front(
        query, keys, values, out_gate, in_gate, forget, doc_ids, head_gain, w_out, resid, ffn_gain,
        w_gate.T, w_value.T,
    )
    w_down, gate_both = lax.optimization_barrier((w_down, gate_both))
    down_own = lax.dynamic_slice_in_dim(w_down, side * half, half, 0)
    down_other = lax.dynamic_slice_in_dim(w_down, (1 - side) * half, half, 0)

    def collect(own, other):
        near = flip(other, across)
        far = flip(own, 2 * across)
        far_near = flip(near, 2 * across)
        blocks = []
        for block, bits in (
            (own, 0),
            (near, across),
            (far, 2 * across),
            (far_near, 3 * across),
        ):
            blocks.append((block, me ^ bits))
            for by in range(1, across):
                source = me - column + (column - by + across) % across
                blocks.append((shift(block, by), source ^ bits))
        return blocks

    down_blocks = collect(down_own, down_other)
    local_cols = resid.shape[1]
    masks, masks_theirs = masks_both[0, :2], masks_both[1, :2]
    gate_mine, gate_theirs = gate_both[:tokens], gate_both[tokens:]
    edge_mine, edge_theirs = gate_mine[-2:], gate_theirs[-2:]
    edge_low = jnp.where(first, edge_mine, edge_theirs)
    edge_high = jnp.where(first, edge_theirs, edge_mine)
    got_low = shift(edge_low, 1)
    got_high = lax.ppermute(edge_high, "sp", next_pairs(count, across))
    swap = column == 0
    prev_low = jnp.where(swap, got_high, got_low)
    prev_high = jnp.where(swap, got_low, got_high)
    prev_mine = jnp.where(first, prev_low, prev_high)
    prev_theirs = jnp.where(first, prev_high, prev_low)

    taps_low, taps_high = conv_taps[:, :half], conv_taps[:, half:]
    taps = jnp.where(first, taps_low, taps_high)

    def mixed(gate, value, prev, mask):
        extended = jnp.concatenate([prev, gate], axis=0).astype(jnp.float32)
        near = mask[0][:, None] > 0.5
        far = mask[1][:, None] > 0.5
        conv = (
            taps[2] * extended[2:]
            + taps[1] * jnp.where(near, extended[1:-1], 0.0)
            + taps[0] * jnp.where(far, extended[:-2], 0.0)
        )
        return (jax.nn.silu(conv) * value.astype(jnp.float32)).astype(jnp.bfloat16)

    def lowered(gate, value, prev, mask):
        terms = down_product(mixed(gate, value, prev, mask), down_blocks)
        share = lax.psum_scatter(terms, "tp", scatter_dimension=0, tiled=True)
        return share.transpose(1, 0, 2).reshape(tokens, local_cols)

    down_theirs = flip(lowered(gate_theirs, value_both[tokens:], prev_theirs, masks_theirs), across)
    down_mine = lowered(gate_mine, value_both[:tokens], prev_mine, masks)
    down = down_mine.astype(jnp.float32) + down_theirs.astype(jnp.float32)
    return (residual_own + down).astype(jnp.bfloat16)


def next_pairs(count, across):
    pairs = []
    for s in range(count):
        column, top = s % across, s // (2 * across)
        if column < across - 1:
            pairs.append((s, s + 1))
        elif (top + 1) * 2 * across < count:
            pairs.append((s, s - column + 2 * across))
    return pairs


def solution(mesh):
    placed = (
        P("sp", "tp"),
        P("sp", "tp"),
        P("sp", "tp"),
        P("sp", "tp"),
        P("sp", "tp"),
        P("tp", "sp"),
        P("tp", "sp"),
        P("sp"),
        P("tp"),
        P("tp", None),
        P(),
        P("sp", "tp"),
        P("sp", "tp"),
        P(None, "tp"),
        P("tp", "sp"),
    )
    return jax.shard_map(layer, mesh=mesh, in_specs=placed, out_specs=P("sp", "tp"), check_vma=False)
```

```python
import jax
import jax.numpy as jnp
from jax import lax
from jax.experimental import pallas as pl
from jax.experimental.pallas import tpu as pltpu
from jax.sharding import PartitionSpec as P

MESH = pl.DeviceIdType.MESH
DH = 96
ZS = 4
ABSENT = -1e30
LONGEST = 3072
epsilon = 1e-06
head_floor = 1.0


def fused(query, keys, values, out_gate, in_gate, forget, doc_ids, head_gain, w_out, resid, ffn_gain, wg, wv, taps, w_down):
    tokens, width = query.shape
    heads = in_gate.shape[0]
    own_cols = resid.shape[1]
    n_sp, n_tp = lax.axis_size("sp"), lax.axis_size("tp")
    X, Y = n_sp // ZS, n_tp // 2
    units, depth = wg.shape
    half = units // 2
    merged = depth % 128 == 0 and X * depth == own_cols and half >= tokens and Y == 2
    per = n_sp // n_tp
    full = own_cols * n_tp
    tile = 256 if tokens % 256 == 0 else tokens
    tiles = tokens // tile
    reach = min(n_sp - 1, -(-(LONGEST - 1) // tokens))
    steps = []
    d = 1
    while d < tokens:
        steps.append(d)
        d *= 2
    groups = X // per
    wd_shape = (ZS, half, X * depth) if merged else (ZS, X, half, depth)
    landing = (1, 16, 128) if merged else (4 * Y - 1, tokens, own_cols)
    w_shape = (ZS, 2, half, X * depth) if merged else (ZS, 2, X, half, depth)

    def kernel(
        q_ref, k_ref, v_ref, og_ref, ig_ref, fg_ref, doc_ref, hg_ref, wo_hbm, res_ref, gain_ref, wg_hbm, wv_hbm, taps_ref, wd_hbm,
        out_ref,
        resid_ref, mask_ref, gbuf, wd, land, w, rows, acc, wo, mixes, local, states, infos, small, cols, cols2, pad, carry, sin, sq, sqb,
        z_send, z_recv, x_send, x_recv, own_sem, wo_send, wo_recv, wo_own,
        st_send, st_recv, in_send, in_recv, mix_send, mix_recv, sq_send, sq_recv, ra_send, ra_recv, rb_send, rb_recv, rz_send, rz_recv, mk_send, mk_recv,
        dz_send, dz_recv, dx_send, dx_recv, down_own, ed_send, ed_recv, sb_send, sb_recv, yy_send, yy_recv, zz_send, zz_recv, free,
    ):
        me, t = lax.axis_index("sp"), lax.axis_index("tp")
        z, col = me // X, me % X
        side = z % 2
        y, core = t // 2, t % 2
        sib = t + 1 - 2 * core
        end = z % 3 == 0
        to = [z, z + 1 - 2 * side, (z + 2) % 4, 3 - z]
        zs = [z, to[1], jnp.where(end, to[2], to[3]), jnp.where(end, to[3], to[2])]
        kind = [0, 0, jnp.where(end, 1, 2), jnp.where(end, 2, 1)]
        halves = [side, 1 - side, side, 1 - side]

        def sp_dev(i):
            return {"sp": i, "tp": t}

        def tp_dev(i):
            return {"sp": me, "tp": i}

        barrier = pltpu.get_barrier_semaphore()
        for i in range(1, n_sp):
            pl.semaphore_signal(barrier, inc=1, device_id=sp_dev((me + i) % n_sp), device_id_type=MESH)
        for i in range(1, n_tp):
            pl.semaphore_signal(barrier, inc=1, device_id=tp_dev((t + i) % n_tp), device_id_type=MESH)
        pl.semaphore_wait(barrier, n_sp + n_tp - 2)

        hbm = (wg_hbm, wv_hbm)

        def lanes(c):
            return pl.ds(pl.multiple_of(c * depth, depth), depth)

        def slot(zi, part, c):
            if merged:
                return w.at[zi, part, :, lanes(c)]
            return w.at[zi, part, c]

        def half_of(part, s):
            return hbm[part].at[pl.ds(pl.multiple_of(s * half, 16), half), :]

        def z_copy(j, part):
            return pltpu.make_async_remote_copy(
                src_ref=half_of(part, halves[j]), dst_ref=slot(z, part, col),
                send_sem=z_send.at[j - 1, part], recv_sem=z_recv.at[j - 1, part],
                device_id=sp_dev(to[j] * X + col), device_id_type=MESH)

        def z_wait(j, part):
            there = slot(zs[j], part, col)
            pltpu.make_async_remote_copy(
                src_ref=there, dst_ref=there,
                send_sem=z_send.at[kind[j], part], recv_sem=z_recv.at[kind[j], part],
                device_id=sp_dev(zs[j] * X + col), device_id_type=MESH).wait_recv()

        def x_copy(j, part, by):
            src = half_of(part, side) if j == 0 else slot(zs[j], part, col)
            return pltpu.make_async_remote_copy(
                src_ref=src, dst_ref=slot(zs[j], part, col),
                send_sem=x_send.at[j, part, by - 1], recv_sem=x_recv.at[j, part, by - 1],
                device_id=sp_dev(z * X + (col + by) % X), device_id_type=MESH)

        def x_start(j, part):
            for by in range(1, X):
                x_copy(j, part, by).start()

        def relay(j, part):
            z_wait(j, part)
            x_start(j, part)

        def x_wait(j, part):
            for by in range(1, X):
                there = slot(zs[j], part, (col + X - by) % X)
                pltpu.make_async_remote_copy(
                    src_ref=there, dst_ref=there,
                    send_sem=x_send.at[j, part, by - 1], recv_sem=x_recv.at[j, part, by - 1],
                    device_id=sp_dev(z * X + (col + by) % X), device_id_type=MESH).wait_recv()

        def down_slot(zi, c):
            if merged:
                return wd.at[zi, :, lanes(c)]
            return wd.at[zi, c]

        def down_half(s):
            return wd_hbm.at[pl.ds(pl.multiple_of(s * half, 16), half), :]

        def dz_copy(j):
            return pltpu.make_async_remote_copy(
                src_ref=down_half(halves[j]), dst_ref=down_slot(z, col),
                send_sem=dz_send.at[j - 1], recv_sem=dz_recv.at[j - 1],
                device_id=sp_dev(to[j] * X + col), device_id_type=MESH)

        def dx_copy(j, by):
            src = down_half(side) if j == 0 else down_slot(zs[j], col)
            return pltpu.make_async_remote_copy(
                src_ref=src, dst_ref=down_slot(zs[j], col),
                send_sem=dx_send.at[j, by - 1], recv_sem=dx_recv.at[j, by - 1],
                device_id=sp_dev(z * X + (col + by) % X), device_id_type=MESH)

        def dx_start(j):
            for by in range(1, X):
                dx_copy(j, by).start()

        def down_relay(j):
            there = down_slot(zs[j], col)
            pltpu.make_async_remote_copy(
                src_ref=there, dst_ref=there, send_sem=dz_send.at[kind[j]], recv_sem=dz_recv.at[kind[j]],
                device_id=sp_dev(zs[j] * X + col), device_id_type=MESH).wait_recv()
            dx_start(j)

        def dx_wait(j):
            for by in range(1, X):
                there = down_slot(zs[j], (col + X - by) % X)
                pltpu.make_async_remote_copy(
                    src_ref=there, dst_ref=there, send_sem=dx_send.at[j, by - 1], recv_sem=dx_recv.at[j, by - 1],
                    device_id=sp_dev(z * X + (col + by) % X), device_id_type=MESH).wait_recv()

        z_copy(1, 0).start()
        x_start(0, 0)
        for part in range(2):
            pltpu.make_async_copy(half_of(part, side), slot(z, part, col), own_sem.at[part]).start()

        def wo_cols(i):
            return wo_hbm.at[:, pl.ds(pl.multiple_of(i * own_cols, own_cols), own_cols)]

        def wo_rows(i):
            return wo.at[pl.ds(pl.multiple_of(i * width, 16), width), :]

        def wo_copy(i):
            peer = (t + i) % n_tp
            return pltpu.make_async_remote_copy(
                src_ref=wo_cols(peer), dst_ref=wo_rows(t),
                send_sem=wo_send.at[i - 1], recv_sem=wo_recv.at[i - 1],
                device_id=tp_dev(peer), device_id_type=MESH)

        def wo_wait(i):
            there = wo_rows((t + n_tp - i) % n_tp)
            pltpu.make_async_remote_copy(
                src_ref=there, dst_ref=there, send_sem=wo_send.at[i - 1], recv_sem=wo_recv.at[i - 1],
                device_id=tp_dev((t + i) % n_tp), device_id_type=MESH).wait_recv()

        for i in range(1, n_tp):
            wo_copy(i).start()
        pltpu.make_async_copy(wo_cols(t), wo_rows(t), wo_own).start()

        lane = lax.broadcasted_iota(jnp.int32, (8, tokens), 1)
        pad[...] = jnp.zeros_like(pad)
        small[...] = jnp.zeros_like(small)
        pad[0, 0:heads, :] = ig_ref[...]
        pad[1, 0:heads, :] = fg_ref[...]
        gin, f = pad[0], pad[1]
        c = jnp.minimum(f, 0.0) - jnp.log1p(jnp.exp(-jnp.abs(f)))
        seg = jnp.broadcast_to(doc_ref[...].astype(jnp.float32), (8, tokens))
        for d in steps:
            c = c + jnp.where(lane >= d, pltpu.roll(c, d, 1), 0.0)
        b = gin - c
        m = b
        for d in steps:
            ok = (lane >= d) & (pltpu.roll(seg, d, 1) == seg)
            m = jnp.where(ok, jnp.maximum(m, pltpu.roll(m, d, 1)), m)
        c_last, m_last, s_last = c[:, tokens - 1 :], m[:, tokens - 1 :], seg[:, tokens - 1 :]
        s_second = seg[:, tokens - 2 : tokens - 1]
        weight = jnp.where(seg == s_last, jnp.exp(jnp.minimum(b - m_last, 0.0)), 0.0)
        small[0:8] = m
        small[8:16] = weight
        small[16:24] = seg
        small[24:32] = b
        small[32:40] = c
        cols[...] = small[...].T

        for h in range(heads):
            part = slice(h * DH, (h + 1) * DH)
            weighted = (k_ref[:, part].astype(jnp.float32) * cols[:, 8 + h : 9 + h]).astype(jnp.bfloat16)
            states[me, h * DH : (h + 1) * DH, :] = (lax.dot_general(
                weighted, v_ref[:, part], (((0,), (0,)), ((), ())), preferred_element_type=jnp.float32
            ) * (DH ** -0.5)).astype(jnp.bfloat16)
        infos[me, 0:8, :] = jnp.broadcast_to(c_last + m_last, (8, DH))
        infos[me, 8:16, :] = jnp.broadcast_to(c_last, (8, DH))
        first_lane = lax.broadcasted_iota(jnp.int32, (8, DH), 1) == 0
        infos[me, 16:24, :] = jnp.where(
            first_lane, jnp.broadcast_to(s_last, (8, DH)), jnp.broadcast_to(s_second, (8, DH)))

        def st_copy(d):
            return pltpu.make_async_remote_copy(
                src_ref=states.at[me], dst_ref=states.at[me],
                send_sem=st_send.at[d - 1], recv_sem=st_recv.at[d - 1],
                device_id=sp_dev((me + d) % n_sp), device_id_type=MESH)

        def in_copy(d):
            return pltpu.make_async_remote_copy(
                src_ref=infos.at[me], dst_ref=infos.at[me],
                send_sem=in_send.at[d - 1], recv_sem=in_recv.at[d - 1],
                device_id=sp_dev((me + d) % n_sp), device_id_type=MESH)

        def tell(d):
            in_copy(d).start()
            st_copy(d).start()

        for d in range(1, reach + 1):
            pl.when(me + d < n_sp)(lambda d=d: tell(d))
        z_copy(1, 1).start()
        x_start(0, 1)

        def far(order):
            for j, part in order:
                z_copy(j, part).start()

        pl.when(end)(lambda: far(((2, 0), (2, 1), (3, 0), (3, 1))))
        pl.when(jnp.logical_not(end))(lambda: far(((2, 0), (2, 1), (3, 0), (3, 1))))

        for i in range(tiles):
            span = (i + 1) * tile
            at = slice(i * tile, span)
            tpos = lax.broadcasted_iota(jnp.int32, (tile, span), 0) + i * tile
            spos = lax.broadcasted_iota(jnp.int32, (tile, span), 1)
            allowed = (tpos >= spos) & (cols[at, 16:17] == small[16:17, 0:span])
            for h in range(heads):
                part = slice(h * DH, (h + 1) * DH)
                log = jnp.where(allowed, small[24 + h : 25 + h, 0:span] - cols[at, h : h + 1], ABSENT)
                scores = lax.dot_general(
                    q_ref[at, part], k_ref[0:span, part], (((1,), (1,)), ((), ())), preferred_element_type=jnp.float32)
                scores = (scores * jnp.exp(log)).astype(jnp.bfloat16)
                local[at, part] = jnp.dot(scores, v_ref[0:span, part], preferred_element_type=jnp.float32) * (DH ** -0.5)

        relay(1, 0)

        carry[0] = jnp.zeros((8, DH), jnp.float32)
        carry[1] = jnp.full((8, DH), ABSENT, jnp.float32)
        carry[2] = jnp.full((8, DH), -1.0, jnp.float32)
        sin[...] = jnp.zeros_like(sin)

        def earlier(d):
            source = (me + n_sp - d) % n_sp
            for buf, send, recv in ((infos, in_send, in_recv), (states, st_send, st_recv)):
                there = buf.at[source]
                pltpu.make_async_remote_copy(
                    src_ref=there, dst_ref=there, send_sem=send.at[d - 1], recv_sem=recv.at[d - 1],
                    device_id=sp_dev((me + d) % n_sp), device_id_type=MESH).wait_recv()
            block = infos[source]
            peak, total, ends = block[0:8], block[8:16], block[16:24]
            if d == 1:
                carry[2] = ends
            use = ends[:, 0:1] == carry[2][:, 0:1]
            logs = jnp.where(use, peak + carry[0], ABSENT)
            carry[2 + d] = logs
            carry[1] = jnp.maximum(carry[1], logs)
            carry[0] = carry[0] + total

        for d in range(1, reach + 1):
            pl.when(me >= d)(lambda d=d: earlier(d))


        def add_state(d):
            coef = jnp.exp(carry[2 + d] - carry[1])
            for h in range(heads):
                at = slice(h * DH, (h + 1) * DH)
                sin[at, :] = sin[at, :] + coef[h : h + 1, :] * states[(me + n_sp - d) % n_sp, at, :].astype(jnp.float32)

        for d in range(1, reach + 1):
            pl.when(me >= d)(lambda d=d: add_state(d))

        peak_in = carry[1][:, 0:1]
        last_prev = carry[2][:, 0:1]
        second_prev = carry[2][:, 1:2]
        c, m, seg = small[32:40], small[0:8], small[16:24]
        inter = jnp.where(seg == last_prev, c + peak_in, ABSENT)
        top = c + m
        peak_all = jnp.maximum(inter, top)
        before = jnp.where(lane == 0, last_prev, pltpu.roll(seg, 1, 1))
        before2 = jnp.where(lane == 0, second_prev, jnp.where(lane == 1, last_prev, pltpu.roll(seg, 2, 1)))
        row = lax.broadcasted_iota(jnp.int32, (8, tokens), 0)
        mask_ref[0] = jnp.where(jnp.where(row == 0, before, before2) == seg, 1.0, 0.0)
        small[40:48] = jnp.exp(top - peak_all)
        small[48:56] = jnp.exp(inter - peak_all)
        cols2[...] = small[...].T

        for i in range(tiles):
            at = slice(i * tile, (i + 1) * tile)
            for h in range(heads):
                part = slice(h * DH, (h + 1) * DH)
                out = cols2[at, 40 + h : 41 + h] * local[at, part] + cols2[at, 48 + h : 49 + h] * jnp.dot(
                    q_ref[at, part], sin[part, :].astype(jnp.bfloat16), preferred_element_type=jnp.float32)
                local[at, part] = out * lax.rsqrt(jnp.mean(out * out, axis=-1, keepdims=True) + head_floor)
            mixes[t, at, :] = (
                local[at, :] * hg_ref[...] * jax.nn.sigmoid(og_ref[at, :].astype(jnp.float32))
            ).astype(jnp.bfloat16)

        def gather(at, send, recv):
            def copy(index, source, dest):
                return pltpu.make_async_remote_copy(
                    src_ref=at(source), dst_ref=at(source), send_sem=send.at[index], recv_sem=recv.at[index],
                    device_id=tp_dev(dest), device_id_type=MESH)

            def start():
                copy(0, t, sib).start()
                for j in range(1, Y):
                    copy(j, t, ((y + j) % Y) * 2 + core).start()

            def forward():
                for j in range(1, Y):
                    source = ((y + Y - j) % Y) * 2 + core
                    copy(j, source, sib).wait_recv()
                    copy(Y - 1 + j, source, sib).start()

            def finish():
                copy(0, sib, sib).wait_recv()
                for j in range(1, Y):
                    copy(Y - 1 + j, ((y + Y - j) % Y) * 2 + 1 - core, sib).wait_recv()

            def sent():
                copy(0, t, sib).wait_send()
                for j in range(1, Y):
                    copy(j, t, sib).wait_send()
                    copy(Y - 1 + j, t, sib).wait_send()

            return start, forward, finish, sent

        mix_g = gather(lambda i: mixes.at[i], mix_send, mix_recv)
        mix_g[0]()
        relay(1, 1)
        mix_g[1]()
        for i in range(1, n_tp):
            wo_wait(i)
        pltpu.make_async_copy(wo_cols(t), wo_rows(t), wo_own).wait()
        mix_g[2]()

        def project(i, _):
            at = pl.ds(pl.multiple_of(i * tile, tile), tile)
            total = res_ref[at, :].astype(jnp.float32)
            for s in range(n_tp):
                total = total + jnp.dot(
                    mixes[s, at, :], wo[s * width : (s + 1) * width, :], preferred_element_type=jnp.float32)
            resid_ref[at, :] = total
            cols2[at, :] = jnp.broadcast_to(jnp.sum(total * total, axis=1, keepdims=True), (tile, 128))
            return 0

        lax.fori_loop(0, tiles, project, 0)
        sq[t] = cols2[...].T[0:8]

        def sq_copy(i):
            return pltpu.make_async_remote_copy(
                src_ref=sq.at[t], dst_ref=sq.at[t], send_sem=sq_send.at[i - 1], recv_sem=sq_recv.at[i - 1],
                device_id=tp_dev((t + i) % n_tp), device_id_type=MESH)

        for i in range(1, n_tp):
            sq_copy(i).start()
        for i in range(1, n_tp):
            there = sq.at[(t + n_tp - i) % n_tp]
            pltpu.make_async_remote_copy(
                src_ref=there, dst_ref=there, send_sem=sq_send.at[i - 1], recv_sem=sq_recv.at[i - 1],
                device_id=tp_dev((t + i) % n_tp), device_id_type=MESH).wait_recv()
        squares = sq[0]
        for s in range(1, n_tp):
            squares = squares + sq[s]
        small[0:8] = lax.rsqrt(squares / full + epsilon)
        cols2[...] = small[...].T

        def normalize(i, _):
            at = pl.ds(pl.multiple_of(i * tile, tile), tile)
            rows[t, at, :] = (resid_ref[at, :] * cols2[at, 0:1] * gain_ref[t]).astype(jnp.bfloat16)
            return 0

        lax.fori_loop(0, tiles, normalize, 0)

        mine, theirs = pl.ds(0, tokens), pl.ds(tokens, tokens)
        ra = gather(lambda i: rows.at[i, mine], ra_send, ra_recv)
        rb = gather(lambda i: rows.at[i, theirs], rb_send, rb_recv)
        partner = sp_dev(zs[1] * X + col)
        rz = pltpu.make_async_remote_copy(
            src_ref=rows.at[t, mine], dst_ref=rows.at[t, theirs], send_sem=rz_send, recv_sem=rz_recv,
            device_id=partner, device_id_type=MESH)
        mk = pltpu.make_async_remote_copy(
            src_ref=mask_ref.at[0], dst_ref=mask_ref.at[1], send_sem=mk_send, recv_sem=mk_recv,
            device_id=partner, device_id_type=MESH)
        ra[0]()
        rz.start()
        mk.start()

        def rest():
            for j in (1, 2, 3):
                dz_copy(j).start()

        pl.when(end)(rest)
        def down_all():
            for j in (2, 3, 1):
                dz_copy(j).start()

        pl.when(jnp.logical_not(end))(down_all)
        pltpu.make_async_copy(down_half(side), down_slot(z, col), down_own).start()

        def turn(at_end, inside):
            for cond, pairs in ((end, at_end), (jnp.logical_not(end), inside)):
                def run(pairs=pairs):
                    for j, part in pairs:
                        relay(j, part)

                if pairs:
                    pl.when(cond)(run)

        turn(((2, 0),), ((3, 0),))
        ra[1]()
        turn(((2, 1),), ((2, 0),))
        rz.wait_recv()
        rb[0]()
        ra[2]()
        turn((), ((2, 1),))

        def ready(j):
            for part in range(2):
                if j == 0:
                    pltpu.make_async_copy(half_of(part, side), slot(z, part, col), own_sem.at[part]).wait()
                x_wait(j, part)

        def multiply(j, blocks, begin, end):
            def body(i, _):
                at = pl.ds(pl.multiple_of(i * tile, tile), tile)
                for part in range(2):
                    total = None if begin else acc[part, at, :]
                    for zi in [zs[k] for k in j]:
                        if merged:
                            terms = [(rows[zi, at, :], w[zi, part])]
                        else:
                            terms = [
                                (rows[zi * (X // per) + x // per, at, (x % per) * depth : (x % per + 1) * depth],
                                 w[zi, part, x])
                                for x in range(X)
                            ]
                        for left, right in terms:
                            term = lax.dot_general(
                                left, right, (((1,), (1,)), ((), ())), preferred_element_type=jnp.float32)
                            total = term if total is None else total + term
                    if end and part == 0:
                        place = pl.ds(pl.multiple_of(16 + (i % tiles) * tile, 16), tile)
                        gbuf[i // tiles, place, :] = total.astype(jnp.bfloat16)
                    elif end:
                        acc[part, at, :] = total.astype(jnp.bfloat16).astype(jnp.float32)
                    else:
                        acc[part, at, :] = total
                return 0

            lax.fori_loop(blocks[0] * tiles, blocks[1] * tiles, body, 0)

        ready(0)
        ready(1)
        dx_start(0)
        multiply((0, 1), (0, 1), True, False)
        rb[1]()
        turn((), ((3, 1),))
        rb[2]()
        multiply((0, 1), (1, 2), True, False)
        pl.when(end)(lambda: down_relay(1))
        ready(2)
        multiply((2,), (0, 2), False, False)

        turn(((3, 0), (3, 1)), ())
        ready(3)
        multiply((3,), (0, 2), False, True)

        for part in range(2):
            for j in range(1, 4):
                z_copy(j, part).wait_send()
            for j in range(4):
                for by in range(1, X):
                    x_copy(j, part, by).wait_send()
        ra[3]()
        rb[3]()
        rz.wait_send()
        mk.wait()

        def edge_copy(block, slot_index, dev):
            return pltpu.make_async_remote_copy(
                src_ref=gbuf.at[block, pl.ds(tokens, 16)], dst_ref=gbuf.at[slot_index, pl.ds(0, 16)],
                send_sem=ed_send.at[block], recv_sem=ed_recv.at[slot_index],
                device_id=sp_dev(dev), device_id_type=MESH)

        low, high = side, 1 - side
        inner = col < X - 1

        def edge_low():
            pl.when(inner)(lambda: EDGE(low, low, me + 1))
            pl.when(col == X - 1)(lambda: EDGE(low, high, me + 1 - X))

        def EDGE(block, slot_index, dev):
            edge_copy(block, slot_index, dev).start()

        edge_low()
        pl.when(inner)(lambda: EDGE(high, high, me + 1))
        pl.when((col == X - 1) & (z < 2))(lambda: EDGE(high, low, me + X + 1))

        for dev in [sib] + [((y + j) % Y) * 2 + core for j in range(1, Y)]:
            pl.semaphore_signal(free, inc=1, device_id=tp_dev(dev), device_id_type=MESH)
        pl.semaphore_signal(free, inc=1, device_id=partner, device_id_type=MESH)

        edge_copy(high, high, me).wait_recv()
        pl.when((col > 0) | (z >= 2))(lambda: edge_copy(low, low, me).wait_recv())
        edge_copy(low, low, me).wait_send()
        pl.when(inner | (z < 2))(lambda: edge_copy(high, high, me).wait_send())

        for block in range(2):
            cols2[:, 8 * block : 8 * block + 8] = mask_ref[block].T

        def mix_tile(i, _):
            k = 2 * tiles - 1 - i
            block, first = k // tiles, (k % tiles) * tile
            at = pl.ds(pl.multiple_of(k * tile, tile), tile)
            inside = pl.ds(pl.multiple_of(first, tile), tile)
            ext = gbuf[block, pl.ds(pl.multiple_of(first, 16), tile + 16), :].astype(jnp.float32)
            flags = cols2[inside, 0:16]
            near = jnp.where(block == 0, flags[:, 0:1], flags[:, 8:9]) > 0.5
            far = jnp.where(block == 0, flags[:, 1:2], flags[:, 9:10]) > 0.5
            conv = (
                taps_ref[2:3, :] * ext[16:]
                + taps_ref[1:2, :] * jnp.where(near, ext[15:-1], 0.0)
                + taps_ref[0:1, :] * jnp.where(far, ext[14:-2], 0.0)
            )
            gbuf[block, pl.ds(pl.multiple_of(16 + first, 16), tile), :] = (
                jax.nn.silu(conv) * acc[1, at, :]
            ).astype(jnp.bfloat16)
            return 0

        down_relay(2)
        lax.fori_loop(0, 2 * tiles, mix_tile, 0)

        def span_of(block, i):
            return pl.ds(pl.multiple_of(block * tokens + i * tile, tile), tile)

        def each_tile(do):
            def body(i, _):
                do(tiles - 1 - i)
                return 0

            lax.fori_loop(0, tiles, body, 0)

        def landed(k, i):
            if merged:
                return w.at[k // 2, k % 2, span_of(0, i), :]
            return land.at[k, span_of(0, i)]

        def landed_value(k, at):
            if merged:
                return w[k // 2, k % 2, at, :]
            return land[k, at, :]

        def chunk(g, block, i):
            return rows.at[g, span_of(block, i)]

        def group(j, gx):
            return zs[j] * groups + gx

        def sib_copy(j, gx, block, i):
            g = group(j, gx)
            return pltpu.make_async_remote_copy(
                src_ref=chunk(g, block, i), dst_ref=landed((g // 2) * 2 + block, i),
                send_sem=sb_send.at[j, gx, block, i], recv_sem=sb_recv.at[j, gx, block, i],
                device_id=tp_dev(sib), device_id_type=MESH)

        def y_copy(j, gx, block, i):
            g = group(j, gx)
            jy = (g // 2 - y + Y) % Y
            return pltpu.make_async_remote_copy(
                src_ref=chunk(g, block, i), dst_ref=landed(2 * Y + (jy - 1) * 2 + block, i),
                send_sem=yy_send.at[j, gx, block, i], recv_sem=yy_recv.at[jy - 1, block, i],
                device_id=tp_dev((g // 2) * 2 + core), device_id_type=MESH)

        def zz(i):
            return pltpu.make_async_remote_copy(
                src_ref=chunk(t, 1, i), dst_ref=landed(4 * Y - 2, i), send_sem=zz_send.at[i], recv_sem=zz_recv.at[i],
                device_id=partner, device_id_type=MESH)

        def lower(j, gx):
            g = group(j, gx)

            def body(i, _):
                k = 2 * tiles - 1 - i
                block, first = k // tiles, (k % tiles) * tile
                left = gbuf[block, pl.ds(pl.multiple_of(16 + first, 16), tile), :]
                at = pl.ds(pl.multiple_of(k * tile, tile), tile)
                if merged:
                    rows[g, at, :] = jnp.dot(
                        left, wd[zs[j]], preferred_element_type=jnp.float32).astype(jnp.bfloat16)
                else:
                    for x in range(per):
                        rows[g, at, x * depth : (x + 1) * depth] = jnp.dot(
                            left, wd[zs[j], gx * per + x], preferred_element_type=jnp.float32).astype(jnp.bfloat16)
                pl.when(g % 2 != core)(lambda: sib_copy(j, gx, block, k % tiles).start())
                return 0

            lax.fori_loop(0, 2 * tiles, body, 0)

        def add_into(g, block, slot_index, i):
            place = span_of(block, i)
            rows[g, place, :] = (
                rows[g, place, :].astype(jnp.float32) + landed_value(slot_index, span_of(0, i)).astype(jnp.float32)
            ).astype(jnp.bfloat16)

        def pair_sum(j, gx):
            g = group(j, gx)

            def run():
                for block in (1, 0):
                    def do(i, block=block):
                        sib_copy(j, gx, block, i).wait_recv()
                        add_into(g, block, (g // 2) * 2 + block, i)
                        pl.when(g // 2 != y)(lambda: y_copy(j, gx, block, i).start())

                    each_tile(do)

            pl.when(g % 2 == core)(run)

        every = range(groups)
        pl.semaphore_wait(free, Y + 1)
        pltpu.make_async_copy(down_half(side), down_slot(z, col), down_own).wait()
        dx_wait(0)
        for gx in every:
            lower(0, gx)
        for gx in every:
            pair_sum(0, gx)
        pl.when(jnp.logical_not(end))(lambda: down_relay(1))
        dx_wait(2)
        for gx in every:
            lower(2, gx)
        for gx in every:
            pair_sum(2, gx)
        dx_wait(1)
        for gx in every:
            lower(1, gx)
        for gx in every:
            pair_sum(1, gx)
        down_relay(3)
        dx_wait(3)
        for gx in every:
            lower(3, gx)
        for gx in every:
            pair_sum(3, gx)

        def y_wait(jy, block, i):
            there = landed(2 * Y + (jy - 1) * 2 + block, i)
            pltpu.make_async_remote_copy(
                src_ref=there, dst_ref=there, send_sem=yy_send.at[0, 0, block, i], recv_sem=yy_recv.at[jy - 1, block, i],
                device_id=tp_dev(sib), device_id_type=MESH).wait_recv()

        def give(i):
            for jy in range(1, Y):
                y_wait(jy, 1, i)
                add_into(t, 1, 2 * Y + (jy - 1) * 2 + 1, i)
            zz(i).start()

        def keep(i):
            at = span_of(0, i)
            total = resid_ref[at, :] + rows[t, at, :].astype(jnp.float32)
            for jy in range(1, Y):
                y_wait(jy, 0, i)
                total = total + landed_value(2 * Y + (jy - 1) * 2, at).astype(jnp.float32)
            resid_ref[at, :] = total

        each_tile(give)
        each_tile(keep)

        def finish(i):
            at = span_of(0, i)
            zz(i).wait_recv()
            wo[at, :] = (resid_ref[at, :] + landed_value(4 * Y - 2, at).astype(jnp.float32)).astype(jnp.bfloat16)

        each_tile(finish)
        result = pltpu.make_async_copy(wo.at[pl.ds(0, tokens)], out_ref, wo_own)
        result.start()

        for j in range(1, 4):
            dz_copy(j).wait_send()
        for j in range(4):
            for by in range(1, X):
                dx_copy(j, by).wait_send()
            for gx in every:
                g = group(j, gx)
                for block in range(2):
                    def sib_left(j=j, gx=gx, block=block):
                        each_tile(lambda i: sib_copy(j, gx, block, i).wait_send())

                    def y_left(j=j, gx=gx, block=block):
                        each_tile(lambda i: y_copy(j, gx, block, i).wait_send())

                    pl.when(g % 2 != core)(sib_left)
                    pl.when((g % 2 == core) & (g // 2 != y))(y_left)
        for i in range(1, n_tp):
            wo_copy(i).wait_send()
            sq_copy(i).wait_send()

        def told(d):
            in_copy(d).wait_send()
            st_copy(d).wait_send()

        for d in range(1, reach + 1):
            pl.when(me + d < n_sp)(lambda d=d: told(d))
        mix_g[3]()
        each_tile(lambda i: zz(i).wait_send())
        result.wait()

    vmem = pl.BlockSpec(memory_space=pltpu.VMEM)
    hbm_spec = pl.BlockSpec(memory_space=pl.ANY)
    dma = pltpu.SemaphoreType.DMA
    bf16, f32 = jnp.bfloat16, jnp.float32
    return pl.pallas_call(
        kernel,
        in_specs=[vmem] * 8 + [hbm_spec] + [vmem] * 2 + [hbm_spec] * 2 + [vmem, hbm_spec],
        out_specs=hbm_spec,
        out_shape=jax.ShapeDtypeStruct((tokens, own_cols), bf16),
        scratch_shapes=[
            pltpu.VMEM((tokens, own_cols), f32),
            pltpu.VMEM((2, 8, tokens), f32),
            pltpu.VMEM((2, tokens + 16, half), bf16),
            pltpu.VMEM(wd_shape, bf16),
            pltpu.VMEM(landing, bf16),
            pltpu.VMEM(w_shape, bf16),
            pltpu.VMEM((n_tp, 2 * tokens, own_cols), bf16),
            pltpu.VMEM((2, 2 * tokens, half), f32),
            pltpu.VMEM((n_tp * width, own_cols), bf16),
            pltpu.VMEM((n_tp, tokens, width), bf16),
            pltpu.VMEM((tokens, width), f32),
            pltpu.VMEM((n_sp, heads * DH, DH), bf16),
            pltpu.VMEM((n_sp, 24, DH), f32),
            pltpu.VMEM((128, tokens), f32),
            pltpu.VMEM((tokens, 128), f32),
            pltpu.VMEM((tokens, 128), f32),
            pltpu.VMEM((2, 8, tokens), f32),
            pltpu.VMEM((2 + n_sp, 8, DH), f32),
            pltpu.VMEM((heads * DH, DH), f32),
            pltpu.VMEM((n_tp, 8, tokens), f32),
            pltpu.VMEM((8, 128), f32),
            dma((3, 2)), dma((3, 2)),
            dma((4, 2, X - 1)), dma((4, 2, X - 1)),
            dma((2,)),
            dma((n_tp - 1,)), dma((n_tp - 1,)), dma,
            dma((reach,)), dma((reach,)),
            dma((reach,)), dma((reach,)),
            dma((n_tp - 1,)), dma((n_tp - 1,)),
            dma((n_tp - 1,)), dma((n_tp - 1,)),
            dma((n_tp - 1,)), dma((n_tp - 1,)),
            dma((n_tp - 1,)), dma((n_tp - 1,)),
            dma, dma, dma, dma,
            dma((3,)), dma((3,)),
            dma((4, X - 1)), dma((4, X - 1)), dma,
            dma((2,)), dma((2,)),
            dma((4, groups, 2, tiles)), dma((4, groups, 2, tiles)),
            dma((4, groups, 2, tiles)), dma((Y - 1, 2, tiles)),
            dma((tiles,)), dma((tiles,)),
            pltpu.SemaphoreType.REGULAR,
        ],
        compiler_params=pltpu.CompilerParams(
            vmem_limit_bytes=67043328, collective_id=0, has_side_effects=True),
        name="layer",
    )(
        query, keys, values, out_gate, in_gate, forget, doc_ids[None], head_gain[None], w_out, resid,
        ffn_gain.reshape(n_tp, 1, own_cols), wg, wv, taps, w_down,
    )


def layer(
    resid, query, keys, values, out_gate, in_gate, forget, doc_ids, head_gain,
    w_out, ffn_gain, w_gate, w_value, conv_taps, w_down,
):
    side = (lax.axis_index("sp") // (lax.axis_size("sp") // ZS)) % 2
    half = w_gate.shape[1] // 2
    taps = jnp.where(side == 0, conv_taps[:, :half], conv_taps[:, half:])
    return fused(
        query, keys, values, out_gate, in_gate, forget, doc_ids, head_gain, w_out, resid, ffn_gain,
        w_gate.T, w_value.T, taps, w_down,
    )


def solution(mesh):
    grid = P("sp", "tp")
    placed = (
        grid, grid, grid, grid, grid, P("tp", "sp"), P("tp", "sp"), P("sp"), P("tp"), P("tp", None),
        P(), grid, grid, P(None, "tp"), P("tp", "sp"),
    )
    return jax.shard_map(layer, mesh=mesh, in_specs=placed, out_specs=grid, check_vma=False)
```
